256 devices in a mesh: vp: 32 (over z, x), dp: 8 (over y, core).
Axes of the slice: x: 4, y: 4, z: 8, core: 2. Of those that a mesh axis runs over, the one named last changes fastest.
Arguments:
- hidden_rows: bfloat16 [768, 8, 2048], P('vp', 'dp'), may hold values from -48 to 48
- norm_gain: float32 [2048], replicated, may hold values from 0.1 to 1.9
- vocab_matrix: bfloat16 [2048, 32768], P(None, 'vp'), may hold values from -3 to 3
- vocab_bias: float32 [32768], P('vp'), may hold values from -4 to 4
- targets: int32 [768, 8], P(None, 'dp'), may hold values from 0 to 32767
- loss_weight: float32 [768, 8], P(None, 'dp'), may hold values from 0.5 to 8
Outputs:
- losses: float32 [768, 8], P('vp', 'dp')
- norm_grad: float32 [768, 8, 2048], P('vp', 'dp')
- vocab_grad: float32 [2048, 32768], P('dp', 'vp')
The draws below stay inside these ranges and needn't reach their ends.
All inputs are finite; a program needn't handle non-finite values.
Results may differ from the reference program's by a relative error of at most 0.0056.
Values may be sent and summed in bfloat16 or wider, within the bound.
No kernel may reach another device: no remote copies, remote signals or barrier semaphores. Data moves between devices by JAX's collectives and lax.ppermute only.
A program may use at most 64 MiB of HBM per device.

```python
import math
import jax
import jax.numpy as jnp
import numpy as np
from jax import lax

D = 2048
V_DEV = 1024
TOK_DEV = 768
VOCAB = 32768
TOKENS = 6144
N_DP = 8


def draw_vocab_matrix(key, part):
    matrix = jnp.clip(jax.random.normal(jax.random.fold_in(key, 21), (D, VOCAB), jnp.float32), -6.0, 6.0) * (2.5 / math.sqrt(D))
    return matrix.astype(jnp.bfloat16)


def draw_hidden_rows(key, part):
    inputs = jnp.clip(jax.random.normal(jax.random.fold_in(key, 31), (TOKENS, D), jnp.float32), -6.0, 6.0)
    return inputs.reshape(TOK_DEV, TOKENS // TOK_DEV, D).astype(jnp.bfloat16)


def draw_vocab_bias(key, part):
    shard_ids = jnp.arange(VOCAB, dtype=jnp.int32) // V_DEV
    levels = jax.random.uniform(jax.random.fold_in(key, 41), (VOCAB // V_DEV,), jnp.float32, -1.5, 1.5)
    noise = 0.5 * jnp.clip(jax.random.normal(jax.random.fold_in(key, 42), (VOCAB,), jnp.float32), -4.0, 4.0)
    return levels[shard_ids] + noise


def place_ends(result, rng, smallest, high):
    index_at = [jax.random.randint(jax.random.fold_in(rng, axis), (), 0, length) for axis, length in enumerate(result.shape)]
    longest = result.shape.index(max(result.shape))
    neighbour = index_at[:longest] + [(index_at[longest] + 1) % result.shape[longest]] + index_at[longest + 1:]
    return result.at[tuple(index_at)].set(smallest).at[tuple(neighbour)].set(high)


def block_scale(own_key, extent, cuts, low, top_value):
    level = 1.0
    for dim, blocks in cuts:
        heights = jax.random.uniform(jax.random.fold_in(jax.random.fold_in(own_key, 6), dim), (blocks,), jnp.float32, low / len(cuts), top_value / len(cuts))
        level = level * jnp.repeat(jnp.exp(heights), extent[dim] // blocks).reshape((-1,) + (1,) * (len(extent) - 1 - dim))
    return level


def rank_bounds(amount, skew):
    weights = [(1 << 20) // math.isqrt(grade ** skew) + 1 for grade in range(1, amount + 1)]
    deviation = 1 + sum(weights) // (1 << 30)
    return np.cumsum(np.array([max(1, weight // deviation) for weight in weights]))


def ranked(key, dims, amount, skew):
    grid = rank_bounds(amount, skew)
    pick = jax.random.randint(jax.random.fold_in(key, 1), dims, 0, int(grid[amount - 1]))
    grade = jnp.searchsorted(jnp.asarray(grid, jnp.int32), pick, side="right")
    return jax.random.permutation(jax.random.fold_in(key, 2), amount)[grade].astype(jnp.int32)


def setup_inputs(seed: int = 0) -> dict:
    arg_keys = jax.random.split(jax.random.key(seed), 7)
    hidden_rows = draw_hidden_rows(jax.random.fold_in(arg_keys[6], 71), 0)
    norm_gain = jnp.clip(1.0 + 0.18 * jax.random.normal(arg_keys[1], (D,), jnp.float32), 0.1, 1.9)
    vocab_matrix = draw_vocab_matrix(jax.random.fold_in(arg_keys[6], 71), 0)
    vocab_bias = draw_vocab_bias(jax.random.fold_in(arg_keys[6], 71), 0)
    targets = place_ends(ranked(arg_keys[4], (TOK_DEV, N_DP), VOCAB, 2), jax.random.fold_in(arg_keys[4], 3), 0, VOCAB - 1).astype(jnp.int32)
    loss_weight = jnp.clip(jnp.exp(math.log(8.0) - 2.7725887 * jax.random.uniform(arg_keys[5], (TOK_DEV, N_DP), jnp.float32) ** block_scale(arg_keys[5], (TOK_DEV, N_DP), ((1, 8),), -0.2, 0.2)), 0.5, 8.0)
    return {"hidden_rows": hidden_rows, "norm_gain": norm_gain, "vocab_matrix": vocab_matrix, "vocab_bias": vocab_bias, "targets": targets, "loss_weight": loss_weight}


epsilon = 1e-06
penalty = 0.005

def reference(hidden_rows, norm_gain, vocab_matrix, vocab_bias, targets, loss_weight):
    inputs = hidden_rows.astype(jnp.float32)
    inverse_rms = lax.rsqrt(lax.optimization_barrier(jnp.mean(inputs * inputs, axis=-1, keepdims=True)) + epsilon)
    unit_rows = inputs * inverse_rms
    normed = (unit_rows * norm_gain).astype(jnp.bfloat16)
    column_ids = jnp.arange(VOCAB, dtype=jnp.int32)

    def one_group(carry, group):
        row_block, target_ids, weights = group
        scores = jnp.dot(row_block, vocab_matrix, preferred_element_type=jnp.float32) + vocab_bias[None, :]
        maxima = lax.optimization_barrier(jnp.max(scores, axis=1))
        totals = lax.optimization_barrier(jnp.sum(jnp.exp(scores - maxima[:, None]), axis=1))
        log_total = maxima + jnp.log(totals)
        is_target = column_ids[None, :] == target_ids[:, None]
        target_score = lax.optimization_barrier(jnp.sum(jnp.where(is_target, scores, 0.0), axis=1))
        loss_rows = log_total - target_score + penalty * log_total * log_total
        probs = jnp.exp(scores - log_total[:, None])
        score_grad = (weights[:, None] * ((1.0 + 2.0 * penalty * log_total)[:, None] * probs - jnp.where(is_target, 1.0, 0.0))).astype(jnp.bfloat16)
        row_grad = lax.dot_general(score_grad, vocab_matrix, (((1,), (1,)), ((), ())), preferred_element_type=jnp.float32)
        carry = carry + jnp.dot(row_block.T, score_grad, preferred_element_type=jnp.float32)
        return (carry, (loss_rows, row_grad))
    groups = (jnp.moveaxis(normed, 1, 0), targets.T, loss_weight.T)
    vocab_grad, (loss_groups, grad_groups) = lax.scan(one_group, jnp.zeros((D, VOCAB), jnp.float32), groups)
    row_grad = jnp.moveaxis(grad_groups, 0, 1)
    scaled_grad = norm_gain * row_grad
    norm_grad = inverse_rms * (scaled_grad - unit_rows * lax.optimization_barrier(jnp.mean(scaled_grad * unit_rows, axis=-1, keepdims=True)))
    return (loss_groups.T, norm_grad, vocab_grad)
```

```python
import jax
import jax.numpy as jnp
import numpy as np
from jax import lax
from jax.sharding import Mesh
from jax.sharding import PartitionSpec as P

VP = ("vp_0", "vp_1")
DP = ("dp_0", "dp_1")


epsilon = 1e-06
penalty = 0.005
f32 = jnp.float32
bf16 = jnp.bfloat16

NZ, NX, NY, NC = 8, 4, 4, 2
FAR = (3, 4, 5)


def taken_from(array, axis, step):
    count = lax.axis_size(axis)
    return lax.ppermute(array, axis, [(i, (i - step) % count) for i in range(count)])


def sent_to(array, axis, step):
    return taken_from(array, axis, -step)


def slots(own):
    ring = [(kz, kx) for kz in (2, 6) for kx in range(NX)]
    far = [(kz, kx) for kx in range(NX) for kz in FAR]
    near = [(kz, kx) for kz in (1, 7, 0) for kx in range(NX)]
    return np.array([(kz, kx, r) for kz, kx in ring + far + near for r in range(own)], np.int32)


def three_parts(values):
    high = lax.reduce_precision(values, 8, 7)
    middle = lax.reduce_precision(values - high, 8, 7)
    low = values - high - middle
    return [part.astype(bf16) for part in (high, middle, low)]


def moved(matrix, vectors, dims):
    parts = jnp.stack([part for vector in vectors for part in three_parts(vector)])
    out = lax.dot_general(parts, matrix, (((1,), dims), ((), ())), preferred_element_type=f32)
    return [out[k] + out[k + 1] + out[k + 2] for k in range(0, 3 * len(vectors), 3)]


def local(hidden_rows, norm_gain, vocab_matrix, vocab_bias, targets, loss_weight):
    inputs = hidden_rows[:, 0, :].astype(f32)
    inverse_rms = lax.rsqrt(jnp.mean(inputs * inputs, axis=-1, keepdims=True) + epsilon)
    unit_rows = inputs * inverse_rms
    normed = (unit_rows * norm_gain).astype(bf16)
    own, width = normed.shape
    total_rows = own * NZ * NX
    columns = vocab_matrix.shape[1]

    along_x = {kx: taken_from(normed, "vp_1", kx) for kx in (1, 3, 2)}
    straight = {kz: taken_from(normed, "vp_0", kz) for kz in (4, 3, 5)}
    line = jnp.concatenate([normed] + [along_x[kx] for kx in range(1, NX)])
    up1 = taken_from(line, "vp_0", 1)
    down1 = taken_from(line, "vp_0", -1)
    three = jnp.concatenate([straight[kz] for kz in FAR])
    threes = {kx: taken_from(three, "vp_1", kx) for kx in (2, 1, 3)}
    up2 = taken_from(up1, "vp_0", 1)
    down2 = taken_from(down1, "vp_0", -1)
    rows_all = jnp.concatenate(
        [up2, down2, three] + [threes[kx] for kx in range(1, NX)] + [up1, down1, line]
    )

    place_z, place_x = lax.axis_index("vp_0"), lax.axis_index("vp_1")
    place = slots(own)
    owner = (place_z + place[:, 0]) % NZ * NX + (place_x + place[:, 1]) % NX
    index = owner * own + place[:, 2]
    ids = lax.broadcasted_iota(jnp.int32, (total_rows, total_rows), 1)
    order = (index[:, None] == ids).astype(bf16)

    target_col, weights = moved(
        order, [targets[:, 0].astype(f32), loss_weight[:, 0]], (1,)
    )
    target_col = target_col.astype(jnp.int32) - lax.axis_index(VP) * columns
    column_ids = lax.broadcasted_iota(jnp.int32, (total_rows, columns), 1)
    is_target = column_ids == target_col[:, None]

    scores = jnp.dot(rows_all, vocab_matrix, preferred_element_type=f32) + vocab_bias[None, :]
    maxima = jnp.max(scores, axis=1)
    totals = jnp.sum(jnp.exp(scores - maxima[:, None]), axis=1)
    target_score = jnp.sum(jnp.where(is_target, scores, 0.0), axis=1)
    maxima, totals, target_score = moved(order, [maxima, totals, target_score], (0,))
    count = NZ * NX
    both = jnp.concatenate([maxima, totals])
    target_score = jnp.pad(target_score.reshape(count, own), ((0, 0), (0, 128 - own)))
    packed = jnp.concatenate(
        [jnp.broadcast_to(both, (count, 2 * total_rows)), target_score], axis=1
    )[:, None, :]
    packed = lax.all_to_all(packed, VP, split_axis=0, concat_axis=0, tiled=True)[:, 0]
    each = packed[:, :total_rows]
    maxima = jnp.max(each, axis=0)
    totals = jnp.sum(packed[:, total_rows : 2 * total_rows] * jnp.exp(each - maxima), axis=0)
    log_total = maxima + jnp.log(totals)
    own_log = lax.dynamic_slice_in_dim(log_total, lax.axis_index(VP) * own, own)
    own_target = jnp.sum(packed[:, 2 * total_rows : 2 * total_rows + own], axis=0)
    own_loss = own_log - own_target + penalty * own_log * own_log
    (log_total,) = moved(order, [log_total], (1,))

    probs = jnp.exp(scores - log_total[:, None])
    score_grad = (
        weights[:, None]
        * ((1.0 + 2.0 * penalty * log_total)[:, None] * probs - jnp.where(is_target, 1.0, 0.0))
    ).astype(bf16)

    def row_part(low, high):
        return lax.dot_general(
            score_grad[low:high],
            vocab_matrix,
            (((1,), (1,)), ((), ())),
            preferred_element_type=f32,
        )

    block = NX * own
    wide = len(FAR) * own

    core = lax.axis_index("dp_1")
    share = width // (NY * NC)
    cut = [rows_all[:, k * share : (k + 1) * share] for k in range(NY * NC)]
    even = jnp.concatenate(cut[0::2], axis=1)
    odd = jnp.concatenate(cut[1::2], axis=1)

    def vocab_part(rows):
        return lax.dot_general(
            rows, score_grad, (((0,), (0,)), ((), ())), preferred_element_type=f32
        )

    part2 = row_part(0, 2 * block).astype(bf16)
    from_below = sent_to(part2[:block], "vp_0", 1)
    from_above = sent_to(part2[block:], "vp_0", -1)
    other = taken_from(vocab_part(jnp.where(core == 0, odd, even)).astype(bf16), "dp_1", 1)
    far = row_part(2 * block, 2 * block + NX * wide)
    far_half = far.astype(bf16)
    far_x = {
        kx: sent_to(far_half[kx * wide : (kx + 1) * wide], "vp_1", kx) for kx in (2, 1, 3)
    }
    chip = vocab_part(jnp.where(core == 0, even, odd)) + other.astype(f32)
    chip = chip.reshape(NY, share, columns)
    place_y = lax.axis_index("dp_0")

    def of(k):
        return lax.dynamic_index_in_dim(chip, (place_y + k) % NY, 0, keepdims=False)

    chip_y = {k: sent_to(of(k).astype(bf16), "dp_0", k) for k in (2, 1, 3)}
    part1 = row_part(2 * block + NX * wide, total_rows)
    from_below = sent_to((part1[:block] + from_below.astype(f32)).astype(bf16), "vp_0", 1)
    from_above = sent_to(
        (part1[block : 2 * block] + from_above.astype(f32)).astype(bf16), "vp_0", -1
    )
    far_sum = far[:wide]
    for kx in range(1, NX):
        far_sum = far_sum + far_x[kx].astype(f32)
    far_sum = far_sum.astype(bf16)
    arrived = [
        sent_to(far_sum[k * own : (k + 1) * own], "vp_0", FAR[k]) for k in (1, 0, 2)
    ]
    close = part1[2 * block :] + from_below.astype(f32) + from_above.astype(f32)
    close_half = close.astype(bf16)
    arrived += [
        sent_to(close_half[kx * own : (kx + 1) * own], "vp_1", kx) for kx in (2, 1, 3)
    ]
    row_grad = close[:own]
    for piece in arrived:
        row_grad = row_grad + piece.astype(f32)

    scaled_grad = norm_gain * row_grad
    norm_grad = inverse_rms * (
        scaled_grad - unit_rows * jnp.mean(scaled_grad * unit_rows, axis=-1, keepdims=True)
    )
    vocab_grad = of(0)
    for k in (2, 1, 3):
        vocab_grad = vocab_grad + chip_y[k].astype(f32)
    return (own_loss[:, None], norm_grad[:, None, :], vocab_grad)


def solution(mesh):
    split = Mesh(mesh.devices.reshape(8, 4, 4, 2), ("vp_0", "vp_1", "dp_0", "dp_1"))
    in_specs = (P(VP, DP, None), P(), P(None, VP), P(VP), P(None, DP), P(None, DP))
    out_specs = (P(VP, DP), P(VP, DP, None), P(DP, VP))
    return jax.shard_map(local, mesh=split, in_specs=in_specs, out_specs=out_specs, check_vma=False)
```

```python
import jax
import jax.numpy as jnp
import numpy as np
from jax import lax
from jax.sharding import Mesh
from jax.sharding import PartitionSpec as P


VP = ("vp_0", "vp_1")
DP = ("dp_0", "dp_1")


epsilon = 1e-06
penalty = 0.005
f32 = jnp.float32
bf16 = jnp.bfloat16

NZ, NX, NY, NC = 8, 4, 4, 2
FAR = (3, 4, 5)


def taken_from(array, axis, step):
    count = lax.axis_size(axis)
    return lax.ppermute(array, axis, [(i, (i - step) % count) for i in range(count)])


def sent_to(array, axis, step):
    return taken_from(array, axis, -step)


def slots(own):
    near = [(kz, kx) for kz in (0, 1, 7) for kx in range(NX)]
    far = [(kz, kx) for kx in range(NX) for kz in FAR]
    ring = [(kz, kx) for kz in (2, 6) for kx in range(NX)]
    return np.array([(kz, kx, r) for kz, kx in near + far + ring for r in range(own)], np.int32)


def three_parts(values):
    high = lax.reduce_precision(values, 8, 7)
    middle = lax.reduce_precision(values - high, 8, 7)
    low = values - high - middle
    return [part.astype(bf16) for part in (high, middle, low)]


def moved(matrix, vectors, dims):
    parts = jnp.stack([part for vector in vectors for part in three_parts(vector)])
    out = lax.dot_general(parts, matrix, (((1,), dims), ((), ())), preferred_element_type=f32)
    return [out[k] + out[k + 1] + out[k + 2] for k in range(0, 3 * len(vectors), 3)]


def whole(hidden_rows, norm_gain, vocab_matrix, vocab_bias, targets, loss_weight):
    inputs = hidden_rows[:, 0, :].astype(f32)
    inverse_rms = lax.rsqrt(jnp.mean(inputs * inputs, axis=-1, keepdims=True) + epsilon)
    unit_rows = inputs * inverse_rms
    normed = (unit_rows * norm_gain).astype(bf16)
    own, width = normed.shape
    total_rows = own * NZ * NX
    columns = vocab_matrix.shape[1]

    along_x = {kx: taken_from(normed, "vp_1", kx) for kx in (1, 3, 2)}
    straight = {kz: taken_from(normed, "vp_0", kz) for kz in (4, 3, 5)}
    line = jnp.concatenate([normed] + [along_x[kx] for kx in range(1, NX)])
    up1 = taken_from(line, "vp_0", 1)
    down1 = taken_from(line, "vp_0", -1)
    three = lax.optimization_barrier(jnp.concatenate([straight[kz] for kz in FAR]))
    threes = {kx: taken_from(three, "vp_1", kx) for kx in (2, 1, 3)}
    up2 = taken_from(up1, "vp_0", 1)
    down2 = taken_from(down1, "vp_0", -1)
    rows_all = jnp.concatenate(
        [line, up1, down1, three] + [threes[kx] for kx in range(1, NX)] + [up2, down2]
    )

    place_z, place_x = lax.axis_index("vp_0"), lax.axis_index("vp_1")
    place = slots(own)
    owner = (place_z + place[:, 0]) % NZ * NX + (place_x + place[:, 1]) % NX
    index = owner * own + place[:, 2]
    ids = lax.broadcasted_iota(jnp.int32, (total_rows, total_rows), 1)
    order = (index[:, None] == ids).astype(bf16)

    target_col, weights = moved(
        order, [targets[:, 0].astype(f32), loss_weight[:, 0]], (1,)
    )
    target_col = target_col.astype(jnp.int32) - lax.axis_index(VP) * columns
    column_ids = lax.broadcasted_iota(jnp.int32, (total_rows, columns), 1)
    is_target = column_ids == target_col[:, None]

    scores = jnp.dot(rows_all, vocab_matrix, preferred_element_type=f32) + vocab_bias[None, :]
    maxima = jnp.max(scores, axis=1)
    totals = jnp.sum(jnp.exp(scores - maxima[:, None]), axis=1)
    target_score = jnp.sum(jnp.where(is_target, scores, 0.0), axis=1)
    maxima, totals, target_score = moved(order, [maxima, totals, target_score], (0,))
    count = NZ * NX
    both = jnp.concatenate([maxima, totals])
    target_score = jnp.pad(target_score.reshape(count, own), ((0, 0), (0, 128 - own)))
    packed = jnp.concatenate(
        [jnp.broadcast_to(both, (count, 2 * total_rows)), target_score], axis=1
    )[:, None, :]
    packed = lax.all_to_all(packed, VP, split_axis=0, concat_axis=0, tiled=True)[:, 0]
    each = packed[:, :total_rows]
    maxima = jnp.max(each, axis=0)
    totals = jnp.sum(packed[:, total_rows : 2 * total_rows] * jnp.exp(each - maxima), axis=0)
    log_total = maxima + jnp.log(totals)
    own_log = lax.dynamic_slice_in_dim(log_total, lax.axis_index(VP) * own, own)
    own_target = jnp.sum(packed[:, 2 * total_rows : 2 * total_rows + own], axis=0)
    own_loss = own_log - own_target + penalty * own_log * own_log
    (log_total,) = moved(order, [log_total], (1,))

    probs = jnp.exp(scores - log_total[:, None])
    score_grad = (
        weights[:, None]
        * ((1.0 + 2.0 * penalty * log_total)[:, None] * probs - jnp.where(is_target, 1.0, 0.0))
    ).astype(bf16)

    def row_part(low, high):
        return lax.dot_general(
            score_grad[low:high],
            vocab_matrix,
            (((1,), (1,)), ((), ())),
            preferred_element_type=f32,
        )

    block = NX * own
    wide = len(FAR) * own

    core = lax.axis_index("dp_1")
    share = width // (NY * NC)
    cut = [rows_all[:, k * share : (k + 1) * share] for k in range(NY * NC)]
    even = jnp.concatenate(cut[0::2], axis=1)
    odd = jnp.concatenate(cut[1::2], axis=1)

    def vocab_part(rows):
        return lax.dot_general(
            rows, score_grad, (((0,), (0,)), ((), ())), preferred_element_type=f32
        )

    near_end, far_end = 3 * block, 3 * block + NX * wide
    part2 = row_part(far_end, total_rows).astype(bf16)
    from_below = sent_to(part2[:block], "vp_0", 1)
    from_above = sent_to(part2[block:], "vp_0", -1)
    other = vocab_part(jnp.where(core == 0, odd, even)).astype(bf16)
    other = taken_from(other, "dp_1", 1)
    far = row_part(near_end, far_end)
    far_half = far.astype(bf16)
    far_x = {kx: sent_to(far_half[kx * wide : (kx + 1) * wide], "vp_1", kx) for kx in (2, 1, 3)}
    place_y = lax.axis_index("dp_0")
    chip = vocab_part(jnp.where(core == 0, even, odd)) + other.astype(f32)
    chip = chip.reshape(NY, share, columns)

    def of(k):
        return lax.dynamic_index_in_dim(chip, (place_y + k) % NY, 0, keepdims=False)

    chip_half = {k: of(k).astype(bf16) for k in (2, 1, 3)}
    chip_y = {k: sent_to(chip_half[k], "dp_0", k) for k in (2, 1, 3)}
    part1 = row_part(0, near_end)
    above, below = part1[block : 2 * block], part1[2 * block :]
    from_below = sent_to((above + from_below.astype(f32)).astype(bf16), "vp_0", 1)
    from_above = sent_to((below + from_above.astype(f32)).astype(bf16), "vp_0", -1)
    far_sum = far[:wide]
    for kx in range(1, NX):
        far_sum = far_sum + far_x[kx].astype(f32)
    far_sum = far_sum.astype(bf16)
    arrived = [sent_to(far_sum[k * own : (k + 1) * own], "vp_0", FAR[k]) for k in (1, 0, 2)]
    close = part1[:block] + from_below.astype(f32) + from_above.astype(f32)
    close_half = close.astype(bf16)
    arrived += [sent_to(close_half[kx * own : (kx + 1) * own], "vp_1", kx) for kx in (2, 1, 3)]
    row_grad = close[:own]
    for piece in arrived:
        row_grad = row_grad + piece.astype(f32)

    scaled_grad = norm_gain * row_grad
    norm_grad = inverse_rms * (
        scaled_grad - unit_rows * jnp.mean(scaled_grad * unit_rows, axis=-1, keepdims=True)
    )
    vocab_grad = of(0)
    for k in (2, 1, 3):
        vocab_grad = vocab_grad + chip_y[k].astype(f32)
    return (own_loss[:, None], norm_grad[:, None, :], vocab_grad)


def solution(mesh):
    split = Mesh(mesh.devices.reshape(8, 4, 4, 2), ("vp_0", "vp_1", "dp_0", "dp_1"))
    in_specs = (P(VP, DP, None), P(), P(None, VP), P(VP), P(None, DP), P(None, DP))
    out_specs = (P(VP, DP), P(VP, DP, None), P(DP, VP))
    return jax.shard_map(whole, mesh=split, in_specs=in_specs, out_specs=out_specs, check_vma=False)
```

```python
import jax
import jax.numpy as jnp
import numpy as np
from jax import lax
from jax.sharding import Mesh
from jax.sharding import PartitionSpec as P


VP = ("vp_0", "vp_1")
DP = ("dp_0", "dp_1")


epsilon = 1e-06
penalty = 0.005
f32 = jnp.float32
bf16 = jnp.bfloat16

NZ, NX, NY, NC = 8, 4, 4, 2
FAR = (3, 4, 5)


def taken_from(array, axis, step):
    count = lax.axis_size(axis)
    return lax.ppermute(array, axis, [(i, (i - step) % count) for i in range(count)])


def sent_to(array, axis, step):
    return taken_from(array, axis, -step)


def slots(own):
    near = [(kz, kx) for kz in (0, 1, 7) for kx in range(NX)]
    far = [(kz, kx) for kx in range(NX) for kz in FAR]
    ring = [(kz, kx) for kz in (2, 6) for kx in range(NX)]
    return np.array([(kz, kx, r) for kz, kx in near + far + ring for r in range(own)], np.int32)


def three_parts(values):
    high = lax.reduce_precision(values, 8, 7)
    middle = lax.reduce_precision(values - high, 8, 7)
    low = values - high - middle
    return [part.astype(bf16) for part in (high, middle, low)]


def moved(matrix, vectors, dims):
    parts = jnp.stack([part for vector in vectors for part in three_parts(vector)])
    out = lax.dot_general(parts, matrix, (((1,), dims), ((), ())), preferred_element_type=f32)
    return [out[k] + out[k + 1] + out[k + 2] for k in range(0, 3 * len(vectors), 3)]


def whole(hidden_rows, norm_gain, vocab_matrix, vocab_bias, targets, loss_weight):
    inputs = hidden_rows[:, 0, :].astype(f32)
    inverse_rms = lax.rsqrt(jnp.mean(inputs * inputs, axis=-1, keepdims=True) + epsilon)
    unit_rows = inputs * inverse_rms
    normed = (unit_rows * norm_gain).astype(bf16)
    own, width = normed.shape
    total_rows = own * NZ * NX
    columns = vocab_matrix.shape[1]

    along_x = {kx: taken_from(normed, "vp_1", kx) for kx in (1, 3, 2)}
    straight = {kz: taken_from(normed, "vp_0", kz) for kz in (4, 3, 5)}
    line = jnp.concatenate([normed] + [along_x[kx] for kx in range(1, NX)])
    up1 = taken_from(line, "vp_0", 1)
    down1 = taken_from(line, "vp_0", -1)
    three = lax.optimization_barrier(jnp.concatenate([straight[kz] for kz in FAR]))
    threes = {kx: taken_from(three, "vp_1", kx) for kx in (2, 1, 3)}
    up2 = taken_from(up1, "vp_0", 1)
    down2 = taken_from(down1, "vp_0", -1)
    rows_all = jnp.concatenate(
        [line, up1, down1, three] + [threes[kx] for kx in range(1, NX)] + [up2, down2]
    )

    place_z, place_x = lax.axis_index("vp_0"), lax.axis_index("vp_1")
    place = slots(own)
    owner = (place_z + place[:, 0]) % NZ * NX + (place_x + place[:, 1]) % NX
    index = owner * own + place[:, 2]
    ids = lax.broadcasted_iota(jnp.int32, (total_rows, total_rows), 1)
    order = (index[:, None] == ids).astype(bf16)

    target_col, weights = moved(
        order, [targets[:, 0].astype(f32), loss_weight[:, 0]], (1,)
    )
    target_col = target_col.astype(jnp.int32) - lax.axis_index(VP) * columns
    column_ids = lax.broadcasted_iota(jnp.int32, (total_rows, columns), 1)
    is_target = column_ids == target_col[:, None]

    scores = jnp.dot(rows_all, vocab_matrix, preferred_element_type=f32) + vocab_bias[None, :]
    top = jnp.max(scores, axis=1)
    powers = jnp.exp(scores - top[:, None])
    totals = jnp.sum(powers, axis=1)
    target_score = jnp.sum(jnp.where(is_target, scores, 0.0), axis=1)
    target_power = jnp.sum(jnp.where(is_target, powers, 0.0), axis=1)
    others = jnp.where(is_target, 0.0, powers).astype(bf16)
    maxima, totals, target_score = moved(order, [top, totals, target_score], (0,))
    count = NZ * NX
    both = jnp.concatenate([maxima, totals])
    target_score = jnp.pad(target_score.reshape(count, own), ((0, 0), (0, 128 - own)))
    packed = jnp.concatenate(
        [jnp.broadcast_to(both, (count, 2 * total_rows)), target_score], axis=1
    )[:, None, :]
    packed, others, hot, rows_all = lax.optimization_barrier(
        (packed, others, is_target.astype(bf16), rows_all)
    )
    packed = lax.all_to_all(packed, VP, split_axis=0, concat_axis=0, tiled=True)

    def times_matrix(left):
        return lax.dot_general(
            left, vocab_matrix, (((1,), (1,)), ((), ())), preferred_element_type=f32
        )

    rest = times_matrix(others).astype(bf16)
    hit = times_matrix(hot).astype(bf16)
    core = lax.axis_index("dp_1")
    share = width // (NY * NC)
    cut = [rows_all[:, k * share : (k + 1) * share] for k in range(NY * NC)]
    even = jnp.concatenate(cut[0::2], axis=1)
    odd = jnp.concatenate(cut[1::2], axis=1)
    mine = jnp.where(core == 0, even, odd)
    theirs = jnp.where(core == 0, odd, even)
    packed, rest, hit, mine, theirs = lax.optimization_barrier(
        (packed, rest, hit, mine, theirs)
    )
    packed = packed[:, 0]
    each = packed[:, :total_rows]
    maxima = jnp.max(each, axis=0)
    totals = jnp.sum(packed[:, total_rows : 2 * total_rows] * jnp.exp(each - maxima), axis=0)
    log_total = maxima + jnp.log(totals)
    own_log = lax.dynamic_slice_in_dim(log_total, lax.axis_index(VP) * own, own)
    own_target = jnp.sum(packed[:, 2 * total_rows : 2 * total_rows + own], axis=0)
    own_loss = own_log - own_target + penalty * own_log * own_log
    (log_total,) = moved(order, [log_total], (1,))

    probs = jnp.exp(scores - log_total[:, None])
    score_grad = (
        weights[:, None]
        * ((1.0 + 2.0 * penalty * log_total)[:, None] * probs - jnp.where(is_target, 1.0, 0.0))
    ).astype(bf16)

    scale = weights * (1.0 + 2.0 * penalty * log_total)
    scale_rest = scale * jnp.exp(top - log_total)
    scale_hit = scale_rest * target_power - weights

    def row_part(low, high):
        return (
            scale_rest[low:high, None] * rest[low:high].astype(f32)
            + scale_hit[low:high, None] * hit[low:high].astype(f32)
        )

    def vocab_part(rows):
        return lax.dot_general(
            rows, score_grad, (((0,), (0,)), ((), ())), preferred_element_type=f32
        )

    block = NX * own
    wide = len(FAR) * own
    near_end, far_end = 3 * block, 3 * block + NX * wide
    up, down = far_end, far_end + block
    upward, downward = lax.optimization_barrier(
        (row_part(up, down).astype(bf16), row_part(down, total_rows).astype(bf16))
    )
    from_below = sent_to(upward, "vp_0", 1)
    from_above = sent_to(downward, "vp_0", -1)
    other = vocab_part(theirs).astype(bf16)
    other = taken_from(other, "dp_1", 1)
    far = [near_end + kx * wide for kx in range(NX + 1)]
    far_x = lax.optimization_barrier(
        {kx: row_part(far[kx], far[kx + 1]).astype(bf16) for kx in (2, 1, 3)}
    )
    far_x = {kx: sent_to(far_x[kx], "vp_1", kx) for kx in (2, 1, 3)}
    place_y = lax.axis_index("dp_0")
    chip = vocab_part(mine) + other.astype(f32)
    chip = chip.reshape(NY, share, columns)

    def of(k):
        return lax.dynamic_index_in_dim(chip, (place_y + k) % NY, 0, keepdims=False)

    chip_half = {k: of(k).astype(bf16) for k in (2, 1, 3)}
    chip_y = {k: sent_to(chip_half[k], "dp_0", k) for k in (2, 1, 3)}
    above, below = row_part(block, 2 * block), row_part(2 * block, 3 * block)
    from_below = sent_to((above + from_below.astype(f32)).astype(bf16), "vp_0", 1)
    from_above = sent_to((below + from_above.astype(f32)).astype(bf16), "vp_0", -1)
    far_sum = row_part(far[0], far[1])
    for kx in range(1, NX):
        far_sum = far_sum + far_x[kx].astype(f32)
    far_sum = far_sum.astype(bf16)
    arrived = [sent_to(far_sum[k * own : (k + 1) * own], "vp_0", FAR[k]) for k in (1, 0, 2)]
    close = row_part(0, block) + from_below.astype(f32) + from_above.astype(f32)
    close_half = close.astype(bf16)
    arrived += [sent_to(close_half[kx * own : (kx + 1) * own], "vp_1", kx) for kx in (2, 1, 3)]
    row_grad = close[:own]
    for piece in arrived:
        row_grad = row_grad + piece.astype(f32)

    scaled_grad = norm_gain * row_grad
    norm_grad = inverse_rms * (
        scaled_grad - unit_rows * jnp.mean(scaled_grad * unit_rows, axis=-1, keepdims=True)
    )
    vocab_grad = of(0)
    for k in (2, 1, 3):
        vocab_grad = vocab_grad + chip_y[k].astype(f32)
    return (own_loss[:, None], norm_grad[:, None, :], vocab_grad)


def solution(mesh):
    split = Mesh(mesh.devices.reshape(8, 4, 4, 2), ("vp_0", "vp_1", "dp_0", "dp_1"))
    in_specs = (P(VP, DP, None), P(), P(None, VP), P(VP), P(None, DP), P(None, DP))
    out_specs = (P(VP, DP), P(VP, DP, None), P(DP, VP))
    return jax.shard_map(whole, mesh=split, in_specs=in_specs, out_specs=out_specs, check_vma=False)
```

```python
import jax
import jax.numpy as jnp
import numpy as np
from jax import lax
from jax.experimental import pallas as pl
from jax.experimental.pallas import tpu as pltpu
from jax.sharding import Mesh
from jax.sharding import PartitionSpec as P


VP = ("vp_0", "vp_1")
DP = ("dp_0", "dp_1")


epsilon = 1e-06
penalty = 0.005
f32 = jnp.float32
bf16 = jnp.bfloat16

NZ, NX, NY, NC = 8, 4, 4, 2
FAR = (3, 4, 5)


def taken_from(array, axis, step):
    count = lax.axis_size(axis)
    return lax.ppermute(array, axis, [(i, (i - step) % count) for i in range(count)])


def sent_to(array, axis, step):
    return taken_from(array, axis, -step)


def slots(own):
    near = [(kz, kx) for kz in (0, 1, 7) for kx in range(NX)]
    far = [(kz, kx) for kx in range(NX) for kz in FAR]
    ring = [(kz, kx) for kz in (2, 6) for kx in range(NX)]
    return np.array([(kz, kx, r) for kz, kx in near + far + ring for r in range(own)], np.int32)


def three_parts(values):
    high = lax.reduce_precision(values, 8, 7)
    middle = lax.reduce_precision(values - high, 8, 7)
    low = values - high - middle
    return [part.astype(bf16) for part in (high, middle, low)]


def moved(matrix, vectors, dims):
    parts = jnp.stack([part for vector in vectors for part in three_parts(vector)])
    out = lax.dot_general(parts, matrix, (((1,), dims), ((), ())), preferred_element_type=f32)
    return [out[k] + out[k + 1] + out[k + 2] for k in range(0, 3 * len(vectors), 3)]


def column_vectors(order, vectors):
    high = vectors.astype(bf16)
    left = vectors - high.astype(f32)
    middle = left.astype(bf16)
    low = (left - middle.astype(f32)).astype(bf16)
    return sum(
        lax.dot_general(order, part, (((1,), (1,)), ((), ())), preferred_element_type=f32)
        for part in (high, middle, low)
    )


def gradient_kernel(
    scores, matrix, order, vectors, grad, far_own, near, upward, downward, *far_away
):
    columns = column_vectors(order[...], vectors[...])
    log_total, weights, target = columns[:, 0:1], columns[:, 1:2], columns[:, 2:3]
    scale = weights * (1.0 + 2.0 * penalty * log_total)
    target = target.astype(jnp.int32)
    rows, width = scores.shape
    step = 256
    for low in range(0, width, step):
        part = slice(low, low + step)
        ids = lax.broadcasted_iota(jnp.int32, (rows, step), 1) + low
        probs = jnp.exp(scores[:, part] - log_total)
        grad[:, part] = (
            scale * probs - jnp.where(ids == target, weights, 0.0)
        ).astype(bf16)

    block, wide = upward.shape[0], far_own.shape[0]

    def body(number, carry):
        part = pl.ds(pl.multiple_of(number * step, step), step)
        out = lax.dot_general(
            grad[...], matrix[part, :], (((1,), (1,)), ((), ())), preferred_element_type=f32
        )
        near[:, part] = out[: 3 * block]
        at = 3 * block
        far_own[:, part] = out[at : at + wide]
        for ref in far_away:
            at += wide
            ref[:, part] = out[at : at + wide].astype(bf16)
        at += wide
        upward[:, part] = out[at : at + block].astype(bf16)
        downward[:, part] = out[at + block :].astype(bf16)
        return carry

    lax.fori_loop(0, matrix.shape[0] // step, body, 0)


def vocab_product(rows, grad, first, share):
    part = pl.ds(pl.multiple_of(first * share, share), share)
    return lax.dot_general(
        rows[:, part], grad[...], (((0,), (0,)), ((), ())), preferred_element_type=f32
    )


def other_kernel(place, rows, grad, out):
    share = rows.shape[1] // (NY * NC)

    def body(y, carry):
        product = vocab_product(rows, grad, y * NC + 1 - place[1], share)
        out[pl.ds(pl.multiple_of(y * share, share), share), :] = product.astype(bf16)
        return carry

    lax.fori_loop(0, NY, body, 0)


def chip_kernel(place, rows, grad, other, own, *away):
    share = rows.shape[1] // (NY * NC)
    for k, ref in enumerate((own, *away)):
        y = lax.rem(place[0] + k, NY)
        product = vocab_product(rows, grad, y * NC + place[1], share)
        product = product + other[pl.ds(pl.multiple_of(y * share, share), share), :].astype(f32)
        ref[...] = product.astype(ref.dtype)


def shaped(*shapes):
    return tuple(jax.ShapeDtypeStruct(dims, kind) for dims, kind in shapes)


def spaces(scalars, arrays):
    return [pl.BlockSpec(memory_space=pltpu.SMEM)] * scalars + [
        pl.BlockSpec(memory_space=pltpu.VMEM)
    ] * arrays


def whole(hidden_rows, norm_gain, vocab_matrix, vocab_bias, targets, loss_weight):
    inputs = hidden_rows[:, 0, :].astype(f32)
    inverse_rms = lax.rsqrt(jnp.mean(inputs * inputs, axis=-1, keepdims=True) + epsilon)
    unit_rows = inputs * inverse_rms
    normed = (unit_rows * norm_gain).astype(bf16)
    own, width = normed.shape
    total_rows = own * NZ * NX
    columns = vocab_matrix.shape[1]

    along_x = {kx: taken_from(normed, "vp_1", kx) for kx in (1, 3, 2)}
    straight = {kz: taken_from(normed, "vp_0", kz) for kz in (4, 3, 5)}
    line = jnp.concatenate([normed] + [along_x[kx] for kx in range(1, NX)])
    up1 = taken_from(line, "vp_0", 1)
    down1 = taken_from(line, "vp_0", -1)
    three = lax.optimization_barrier(jnp.concatenate([straight[kz] for kz in FAR]))
    threes = {kx: taken_from(three, "vp_1", kx) for kx in (2, 1, 3)}
    up2 = taken_from(up1, "vp_0", 1)
    down2 = taken_from(down1, "vp_0", -1)
    rows_all = jnp.concatenate(
        [line, up1, down1, three] + [threes[kx] for kx in range(1, NX)] + [up2, down2]
    )

    place_z, place_x = lax.axis_index("vp_0"), lax.axis_index("vp_1")
    place = slots(own)
    owner = (place_z + place[:, 0]) % NZ * NX + (place_x + place[:, 1]) % NX
    index = owner * own + place[:, 2]
    ids = lax.broadcasted_iota(jnp.int32, (total_rows, total_rows), 1)
    order = (index[:, None] == ids).astype(bf16)

    target_col, _ = moved(
        order, [targets[:, 0].astype(f32), loss_weight[:, 0]], (1,)
    )
    target_col = target_col.astype(jnp.int32) - lax.axis_index(VP) * columns
    column_ids = lax.broadcasted_iota(jnp.int32, (total_rows, columns), 1)
    is_target = column_ids == target_col[:, None]

    scores = jnp.dot(rows_all, vocab_matrix, preferred_element_type=f32) + vocab_bias[None, :]
    maxima = jnp.max(scores, axis=1)
    totals = jnp.sum(jnp.exp(scores - maxima[:, None]), axis=1)
    target_score = jnp.sum(jnp.where(is_target, scores, 0.0), axis=1)
    partial_log, target_score = moved(order, [maxima + jnp.log(totals), target_score], (0,))
    count = NZ * NX
    target_score = jnp.pad(target_score.reshape(count, own), ((0, 0), (0, 128 - own)))
    packed = jnp.concatenate(
        [jnp.broadcast_to(partial_log, (count, total_rows)), target_score], axis=1
    )[:, None, :]
    packed = lax.all_to_all(packed, VP, split_axis=0, concat_axis=0, tiled=True)[:, 0]
    each = packed[:, :total_rows]
    maxima = jnp.max(each, axis=0)
    log_total = maxima + jnp.log(jnp.sum(jnp.exp(each - maxima), axis=0))
    own_log = lax.dynamic_slice_in_dim(log_total, lax.axis_index(VP) * own, own)
    own_target = jnp.sum(packed[:, total_rows : total_rows + own], axis=0)
    own_loss = own_log - own_target + penalty * own_log * own_log
    first = lax.axis_index(VP) * columns
    vectors = jnp.concatenate(
        [
            log_total[None],
            loss_weight.T,
            (targets.T - first).astype(f32),
            jnp.zeros((5, total_rows), f32),
        ]
    )
    block = NX * own
    wide = len(FAR) * own
    score_grad, far_own, near, upward, downward, *far_away = pl.pallas_call(
        gradient_kernel,
        out_shape=shaped(
            ((total_rows, columns), bf16),
            ((wide, width), f32),
            ((3 * block, width), f32),
            ((block, width), bf16),
            ((block, width), bf16),
            *[((wide, width), bf16)] * (NX - 1),
        ),
        in_specs=spaces(0, 4),
        out_specs=spaces(0, 5 + NX - 1),
    )(scores, vocab_matrix, order, vectors)
    from_below = sent_to(upward, "vp_0", 1)
    from_above = sent_to(downward, "vp_0", -1)
    far_x = {kx: sent_to(far_away[kx - 1], "vp_1", kx) for kx in (2, 1, 3)}

    share = width // (NY * NC)
    place = jnp.stack([lax.axis_index("dp_0"), lax.axis_index("dp_1")])
    (other,) = pl.pallas_call(
        other_kernel,
        out_shape=shaped(((NY * share, columns), bf16)),
        in_specs=spaces(1, 2),
        out_specs=spaces(0, 1),
    )(place, rows_all, score_grad)
    other = taken_from(other, "dp_1", 1)
    vocab_grad, *away = pl.pallas_call(
        chip_kernel,
        out_shape=shaped(
            ((share, columns), f32), *[((share, columns), bf16)] * (NY - 1)
        ),
        in_specs=spaces(1, 3),
        out_specs=spaces(0, NY),
    )(place, rows_all, score_grad, other)
    chip_y = {k: sent_to(away[k - 1], "dp_0", k) for k in (2, 1, 3)}
    above, below = near[block : 2 * block], near[2 * block :]
    from_below = sent_to((above + from_below.astype(f32)).astype(bf16), "vp_0", 1)
    from_above = sent_to((below + from_above.astype(f32)).astype(bf16), "vp_0", -1)
    far_sum = far_own
    for kx in range(1, NX):
        far_sum = far_sum + far_x[kx].astype(f32)
    far_sum = far_sum.astype(bf16)
    arrived = [sent_to(far_sum[k * own : (k + 1) * own], "vp_0", FAR[k]) for k in (1, 0, 2)]
    close = near[:block] + from_below.astype(f32) + from_above.astype(f32)
    close_half = close.astype(bf16)
    arrived += [sent_to(close_half[kx * own : (kx + 1) * own], "vp_1", kx) for kx in (2, 1, 3)]
    row_grad = close[:own]
    for piece in arrived:
        row_grad = row_grad + piece.astype(f32)

    scaled_grad = norm_gain * row_grad
    norm_grad = inverse_rms * (
        scaled_grad - unit_rows * jnp.mean(scaled_grad * unit_rows, axis=-1, keepdims=True)
    )
    for k in (2, 1, 3):
        vocab_grad = vocab_grad + chip_y[k].astype(f32)
    return (own_loss[:, None], norm_grad[:, None, :], vocab_grad)


def solution(mesh):
    split = Mesh(mesh.devices.reshape(8, 4, 4, 2), ("vp_0", "vp_1", "dp_0", "dp_1"))
    in_specs = (P(VP, DP, None), P(), P(None, VP), P(VP), P(None, DP), P(None, DP))
    out_specs = (P(VP, DP), P(VP, DP, None), P(DP, VP))
    return jax.shard_map(whole, mesh=split, in_specs=in_specs, out_specs=out_specs, check_vma=False)
```

```python
import jax
import jax.numpy as jnp
import numpy as np
from jax import lax
from jax.experimental import pallas as pl
from jax.experimental.pallas import tpu as pltpu
from jax.sharding import Mesh
from jax.sharding import PartitionSpec as P


VP = ("vp_0", "vp_1")
DP = ("dp_0", "dp_1")


epsilon = 1e-06
penalty = 0.005
f32 = jnp.float32
bf16 = jnp.bfloat16

NZ, NX, NY, NC = 8, 4, 4, 2
FAR = (3, 4, 5)


def taken_from(array, axis, step):
    count = lax.axis_size(axis)
    return lax.ppermute(array, axis, [(i, (i - step) % count) for i in range(count)])


def sent_to(array, axis, step):
    return taken_from(array, axis, -step)


def slots(own):
    near = [(kz, kx) for kz in (0, 1, 7) for kx in range(NX)]
    far = [(kz, kx) for kx in range(NX) for kz in FAR]
    ring = [(kz, kx) for kz in (2, 6) for kx in range(NX)]
    return np.array([(kz, kx, r) for kz, kx in near + far + ring for r in range(own)], np.int32)


def three_parts(values):
    high = lax.reduce_precision(values, 8, 7)
    middle = lax.reduce_precision(values - high, 8, 7)
    low = values - high - middle
    return [part.astype(bf16) for part in (high, middle, low)]


def moved(matrix, vectors, dims):
    parts = jnp.stack([part for vector in vectors for part in three_parts(vector)])
    out = lax.dot_general(parts, matrix, (((1,), dims), ((), ())), preferred_element_type=f32)
    return [out[k] + out[k + 1] + out[k + 2] for k in range(0, 3 * len(vectors), 3)]


def column_vectors(order, vectors):
    high = vectors.astype(bf16)
    left = vectors - high.astype(f32)
    middle = left.astype(bf16)
    low = (left - middle.astype(f32)).astype(bf16)
    count = vectors.shape[0]
    parts = jnp.concatenate([high.astype(f32), middle.astype(f32), low.astype(f32)])
    moved_parts = lax.dot_general(
        order, parts.astype(bf16), (((1,), (1,)), ((), ())), preferred_element_type=f32
    )
    return [
        sum(moved_parts[:, k + count * part : k + count * part + 1] for part in range(3))
        for k in range(3)
    ]


def gradient_kernel(
    scores, matrix, order, vectors, grad, far_own, near, upward, downward, *far_away
):
    @pl.when(pl.program_id(0) == 0)
    def first():
        log_total, weights, target = column_vectors(order[...], vectors[...])
        scale = weights * (1.0 + 2.0 * penalty * log_total)
        target = target.astype(jnp.int32)
        rows, width = scores.shape
        step = 128
        for low in range(0, width, step):
            part = slice(low, low + step)
            ids = lax.broadcasted_iota(jnp.int32, (rows, step), 1) + low
            probs = jnp.exp(scores[:, part] - log_total)
            grad[:, part] = (
                scale * probs - jnp.where(ids == target, weights, 0.0)
            ).astype(bf16)

    block, wide = upward.shape[0], far_own.shape[0]
    out = lax.dot_general(
        grad[...], matrix[...], (((1,), (1,)), ((), ())), preferred_element_type=f32
    )
    near[...] = out[: 3 * block]
    at = 3 * block
    far_own[...] = out[at : at + wide]
    for ref in far_away:
        at += wide
        ref[...] = out[at : at + wide].astype(bf16)
    at += wide
    upward[...] = out[at : at + block].astype(bf16)
    downward[...] = out[at + block :].astype(bf16)


def gradients(scores, matrix, order, vectors, block, wide):
    rows, columns = scores.shape
    width = matrix.shape[0]
    step = 512
    kinds = [(wide, f32), (3 * block, f32), (block, bf16), (block, bf16)]
    kinds += [(wide, bf16)] * (NX - 1)
    return pl.pallas_call(
        gradient_kernel,
        grid=(width // step,),
        out_shape=[jax.ShapeDtypeStruct((rows, columns), bf16)]
        + [jax.ShapeDtypeStruct((count, width), kind) for count, kind in kinds],
        in_specs=[
            pl.BlockSpec(scores.shape, lambda i: (0, 0)),
            pl.BlockSpec((step, columns), lambda i: (i, 0)),
            pl.BlockSpec(order.shape, lambda i: (0, 0)),
            pl.BlockSpec(vectors.shape, lambda i: (0, 0)),
        ],
        out_specs=[pl.BlockSpec((rows, columns), lambda i: (0, 0))]
        + [pl.BlockSpec((count, step), lambda i: (0, i)) for count, kind in kinds],
    )(scores, matrix, order, vectors)


def product_over_tokens(rows, grad):
    return lax.dot_general(
        rows[...], grad[...], (((0,), (0,)), ((), ())), preferred_element_type=f32
    )


def other_kernel(place, rows, grad, out):
    out[...] = product_over_tokens(rows, grad).astype(bf16)


def chip_kernel(place, rows, grad, other, own, *away):
    product = product_over_tokens(rows, grad) + other[...].astype(f32)
    for k, ref in enumerate((own, *away)):

        @pl.when(pl.program_id(0) == NY - 1 - k)
        def store(ref=ref):
            ref[...] = product.astype(ref.dtype)


def other_product(place, rows, grad):
    share = rows.shape[1] // (NY * NC)
    tokens, columns = grad.shape
    return pl.pallas_call(
        other_kernel,
        out_shape=jax.ShapeDtypeStruct((NY * share, columns), bf16),
        grid_spec=pltpu.PrefetchScalarGridSpec(
            num_scalar_prefetch=1,
            grid=(NY,),
            in_specs=[
                pl.BlockSpec((tokens, share), lambda y, place: (0, y * NC + 1 - place[1])),
                pl.BlockSpec((tokens, columns), lambda y, place: (0, 0)),
            ],
            out_specs=pl.BlockSpec((share, columns), lambda y, place: (y, 0)),
        ),
    )(place, rows, grad)


def chip_products(place, rows, grad, other):
    share = rows.shape[1] // (NY * NC)
    tokens, columns = grad.shape

    def at(step, place):
        return lax.rem(place[0] + NY - 1 - step, NY)

    return pl.pallas_call(
        chip_kernel,
        out_shape=[jax.ShapeDtypeStruct((share, columns), f32)]
        + [jax.ShapeDtypeStruct((share, columns), bf16)] * (NY - 1),
        grid_spec=pltpu.PrefetchScalarGridSpec(
            num_scalar_prefetch=1,
            grid=(NY,),
            in_specs=[
                pl.BlockSpec(
                    (tokens, share), lambda step, place: (0, at(step, place) * NC + place[1])
                ),
                pl.BlockSpec((tokens, columns), lambda step, place: (0, 0)),
                pl.BlockSpec((share, columns), lambda step, place: (at(step, place), 0)),
            ],
            out_specs=[pl.BlockSpec((share, columns), lambda step, place: (0, 0))] * NY,
        ),
    )(place, rows, grad, other)


def whole(hidden_rows, norm_gain, vocab_matrix, vocab_bias, targets, loss_weight):
    inputs = hidden_rows[:, 0, :].astype(f32)
    inverse_rms = lax.rsqrt(jnp.mean(inputs * inputs, axis=-1, keepdims=True) + epsilon)
    unit_rows = inputs * inverse_rms
    normed = (unit_rows * norm_gain).astype(bf16)
    own, _ = normed.shape
    total_rows = own * NZ * NX
    columns = vocab_matrix.shape[1]

    along_x = {kx: taken_from(normed, "vp_1", kx) for kx in (1, 3, 2)}
    straight = {kz: taken_from(normed, "vp_0", kz) for kz in (4, 3, 5)}
    line = jnp.concatenate([normed] + [along_x[kx] for kx in range(1, NX)])
    up1 = taken_from(line, "vp_0", 1)
    down1 = taken_from(line, "vp_0", -1)
    three = lax.optimization_barrier(jnp.concatenate([straight[kz] for kz in FAR]))
    threes = {kx: taken_from(three, "vp_1", kx) for kx in (2, 1, 3)}
    up2 = taken_from(up1, "vp_0", 1)
    down2 = taken_from(down1, "vp_0", -1)
    rows_all = jnp.concatenate(
        [line, up1, down1, three] + [threes[kx] for kx in range(1, NX)] + [up2, down2]
    )

    place_z, place_x = lax.axis_index("vp_0"), lax.axis_index("vp_1")
    place = slots(own)
    owner = (place_z + place[:, 0]) % NZ * NX + (place_x + place[:, 1]) % NX
    index = owner * own + place[:, 2]
    ids = lax.broadcasted_iota(jnp.int32, (total_rows, total_rows), 1)
    order = (index[:, None] == ids).astype(bf16)

    target_col, _ = moved(
        order, [targets[:, 0].astype(f32), loss_weight[:, 0]], (1,)
    )
    target_col = target_col.astype(jnp.int32) - lax.axis_index(VP) * columns
    column_ids = lax.broadcasted_iota(jnp.int32, (total_rows, columns), 1)
    is_target = column_ids == target_col[:, None]

    scores = jnp.dot(rows_all, vocab_matrix, preferred_element_type=f32) + vocab_bias[None, :]
    maxima = jnp.max(scores, axis=1)
    totals = jnp.sum(jnp.exp(scores - maxima[:, None]), axis=1)
    target_score = jnp.sum(jnp.where(is_target, scores, 0.0), axis=1)
    partial_log, target_score = moved(order, [maxima + jnp.log(totals), target_score], (0,))
    count = NZ * NX
    target_score = jnp.pad(target_score.reshape(count, own), ((0, 0), (0, 128 - own)))
    packed = jnp.concatenate(
        [jnp.broadcast_to(partial_log, (count, total_rows)), target_score], axis=1
    )[:, None, :]
    packed = lax.all_to_all(packed, VP, split_axis=0, concat_axis=0, tiled=True)[:, 0]
    each = packed[:, :total_rows]
    maxima = jnp.max(each, axis=0)
    log_total = maxima + jnp.log(jnp.sum(jnp.exp(each - maxima), axis=0))
    own_log = lax.dynamic_slice_in_dim(log_total, lax.axis_index(VP) * own, own)
    own_target = jnp.sum(packed[:, total_rows : total_rows + own], axis=0)
    own_loss = own_log - own_target + penalty * own_log * own_log
    first = lax.axis_index(VP) * columns
    vectors = jnp.concatenate(
        [
            log_total[None],
            loss_weight.T,
            (targets.T - first).astype(f32),
            jnp.zeros((5, total_rows), f32),
        ]
    )
    block = NX * own
    wide = len(FAR) * own
    score_grad, far_own, near, upward, downward, *far_away = gradients(
        scores, vocab_matrix, order, vectors, block, wide
    )
    from_below = sent_to(upward, "vp_0", 1)
    from_above = sent_to(downward, "vp_0", -1)
    far_x = {kx: sent_to(far_away[kx - 1], "vp_1", kx) for kx in (2, 1, 3)}

    place = jnp.stack([lax.axis_index("dp_0"), lax.axis_index("dp_1")])
    other = other_product(place, rows_all, score_grad)
    other = taken_from(other, "dp_1", 1)
    vocab_grad, *away = chip_products(place, rows_all, score_grad, other)
    chip_y = {k: sent_to(away[k - 1], "dp_0", k) for k in (2, 1, 3)}
    above, below = near[block : 2 * block], near[2 * block :]
    from_below = sent_to((above + from_below.astype(f32)).astype(bf16), "vp_0", 1)
    from_above = sent_to((below + from_above.astype(f32)).astype(bf16), "vp_0", -1)
    far_sum = far_own
    for kx in range(1, NX):
        far_sum = far_sum + far_x[kx].astype(f32)
    far_sum = far_sum.astype(bf16)
    arrived = [sent_to(far_sum[k * own : (k + 1) * own], "vp_0", FAR[k]) for k in (1, 0, 2)]
    close = near[:block] + from_below.astype(f32) + from_above.astype(f32)
    close_half = close.astype(bf16)
    arrived += [sent_to(close_half[kx * own : (kx + 1) * own], "vp_1", kx) for kx in (2, 1, 3)]
    row_grad = close[:own]
    for piece in arrived:
        row_grad = row_grad + piece.astype(f32)

    scaled_grad = norm_gain * row_grad
    norm_grad = inverse_rms * (
        scaled_grad - unit_rows * jnp.mean(scaled_grad * unit_rows, axis=-1, keepdims=True)
    )
    for k in (2, 1, 3):
        vocab_grad = vocab_grad + chip_y[k].astype(f32)
    return (own_loss[:, None], norm_grad[:, None, :], vocab_grad)


def solution(mesh):
    split = Mesh(mesh.devices.reshape(8, 4, 4, 2), ("vp_0", "vp_1", "dp_0", "dp_1"))
    in_specs = (P(VP, DP, None), P(), P(None, VP), P(VP), P(None, DP), P(None, DP))
    out_specs = (P(VP, DP), P(VP, DP, None), P(DP, VP))
    return jax.shard_map(whole, mesh=split, in_specs=in_specs, out_specs=out_specs, check_vma=False)
```

```python
import jax
import jax.numpy as jnp
import numpy as np
from jax import lax
from jax.experimental import pallas as pl
from jax.experimental.pallas import tpu as pltpu
from jax.sharding import Mesh
from jax.sharding import PartitionSpec as P


VP = ("vp_0", "vp_1")
DP = ("dp_0", "dp_1")


epsilon = 1e-06
penalty = 0.005
f32 = jnp.float32
bf16 = jnp.bfloat16

NZ, NX, NY, NC = 8, 4, 4, 2
FAR = (3, 4, 5)


def taken_from(array, axis, step):
    count = lax.axis_size(axis)
    return lax.ppermute(array, axis, [(i, (i - step) % count) for i in range(count)])


def sent_to(array, axis, step):
    return taken_from(array, axis, -step)


def slots(own):
    near = [(kz, kx) for kz in (0, 1, 7) for kx in range(NX)]
    far = [(kz, kx) for kx in range(NX) for kz in FAR]
    ring = [(kz, kx) for kz in (2, 6) for kx in range(NX)]
    return np.array([(kz, kx, r) for kz, kx in near + far + ring for r in range(own)], np.int32)


def three_parts(values):
    high = lax.reduce_precision(values, 8, 7)
    middle = lax.reduce_precision(values - high, 8, 7)
    low = values - high - middle
    return [part.astype(bf16) for part in (high, middle, low)]


def moved(matrix, vectors, dims):
    parts = jnp.stack([part for vector in vectors for part in three_parts(vector)])
    out = lax.dot_general(parts, matrix, (((1,), dims), ((), ())), preferred_element_type=f32)
    return [out[k] + out[k + 1] + out[k + 2] for k in range(0, 3 * len(vectors), 3)]


def column_vectors(order, vectors):
    high = vectors.astype(bf16)
    left = vectors - high.astype(f32)
    middle = left.astype(bf16)
    low = (left - middle.astype(f32)).astype(bf16)
    count = vectors.shape[0]
    parts = jnp.concatenate([high.astype(f32), middle.astype(f32), low.astype(f32)])
    moved_parts = lax.dot_general(
        order, parts.astype(bf16), (((1,), (1,)), ((), ())), preferred_element_type=f32
    )
    return [
        sum(moved_parts[:, k + count * part : k + count * part + 1] for part in range(3))
        for k in range(3)
    ]


def gradient_kernel(
    scores, matrix, order, vectors, grad, far_own, near, upward, downward, *far_away
):
    log_total, weights, target = column_vectors(order[...], vectors[...])
    scale = weights * (1.0 + 2.0 * penalty * log_total)
    target = target.astype(jnp.int32)
    rows, width = scores.shape
    step = 128
    for low in range(0, width, step):
        part = slice(low, low + step)
        ids = lax.broadcasted_iota(jnp.int32, (rows, step), 1) + low
        probs = jnp.exp(scores[:, part] - log_total)
        grad[:, part] = (
            scale * probs - jnp.where(ids == target, weights, 0.0)
        ).astype(bf16)

    block, wide = upward.shape[0], far_own.shape[0]
    step = 512

    def body(number, carry):
        part = pl.ds(pl.multiple_of(number * step, step), step)
        out = lax.dot_general(
            grad[...], matrix[part, :], (((1,), (1,)), ((), ())), preferred_element_type=f32
        )
        near[:, part] = out[: 3 * block]
        at = 3 * block
        far_own[:, part] = out[at : at + wide]
        for ref in far_away:
            at += wide
            ref[:, part] = out[at : at + wide].astype(bf16)
        at += wide
        upward[:, part] = out[at : at + block].astype(bf16)
        downward[:, part] = out[at + block :].astype(bf16)
        return carry

    lax.fori_loop(0, matrix.shape[0] // step, body, 0)


def vocab_product(rows, grad, first, share):
    part = pl.ds(pl.multiple_of(first * share, share), share)
    return lax.dot_general(
        rows[:, part], grad[...], (((0,), (0,)), ((), ())), preferred_element_type=f32
    )


def other_kernel(place, rows, grad, out):
    share = rows.shape[1] // (NY * NC)

    def body(y, carry):
        product = vocab_product(rows, grad, y * NC + 1 - place[1], share)
        out[pl.ds(pl.multiple_of(y * share, share), share), :] = product.astype(bf16)
        return carry

    lax.fori_loop(0, NY, body, 0)


def chip_kernel(place, rows, grad, other, own, *away):
    share = rows.shape[1] // (NY * NC)
    for k, ref in enumerate((own, *away)):
        y = lax.rem(place[0] + k, NY)
        product = vocab_product(rows, grad, y * NC + place[1], share)
        product = product + other[pl.ds(pl.multiple_of(y * share, share), share), :].astype(f32)
        ref[...] = product.astype(ref.dtype)


SMALL = pltpu.CompilerParams(vmem_limit_bytes=8 * 2**20)


def shaped(*shapes):
    return tuple(jax.ShapeDtypeStruct(dims, kind) for dims, kind in shapes)


def spaces(scalars, arrays):
    return [pl.BlockSpec(memory_space=pltpu.SMEM)] * scalars + [
        pl.BlockSpec(memory_space=pltpu.VMEM)
    ] * arrays


def whole(hidden_rows, norm_gain, vocab_matrix, vocab_bias, targets, loss_weight):
    inputs = hidden_rows[:, 0, :].astype(f32)
    inverse_rms = lax.rsqrt(jnp.mean(inputs * inputs, axis=-1, keepdims=True) + epsilon)
    unit_rows = inputs * inverse_rms
    normed = (unit_rows * norm_gain).astype(bf16)
    own, width = normed.shape
    total_rows = own * NZ * NX
    columns = vocab_matrix.shape[1]

    along_x = {kx: taken_from(normed, "vp_1", kx) for kx in (1, 3, 2)}
    straight = {kz: taken_from(normed, "vp_0", kz) for kz in (4, 3, 5)}
    line = jnp.concatenate([normed] + [along_x[kx] for kx in range(1, NX)])
    up1 = taken_from(line, "vp_0", 1)
    down1 = taken_from(line, "vp_0", -1)
    three = lax.optimization_barrier(jnp.concatenate([straight[kz] for kz in FAR]))
    threes = {kx: taken_from(three, "vp_1", kx) for kx in (2, 1, 3)}
    up2 = taken_from(up1, "vp_0", 1)
    down2 = taken_from(down1, "vp_0", -1)
    early = [line, up1, down1, three] + [threes[kx] for kx in range(1, NX)]
    rows_all = jnp.concatenate(
        lax.optimization_barrier(early) + [up2, down2]
    )

    place_z, place_x = lax.axis_index("vp_0"), lax.axis_index("vp_1")
    place = slots(own)
    owner = (place_z + place[:, 0]) % NZ * NX + (place_x + place[:, 1]) % NX
    index = owner * own + place[:, 2]
    ids = lax.broadcasted_iota(jnp.int32, (total_rows, total_rows), 1)
    order = (index[:, None] == ids).astype(bf16)

    target_col, _ = moved(
        order, [targets[:, 0].astype(f32), loss_weight[:, 0]], (1,)
    )
    target_col = target_col.astype(jnp.int32) - lax.axis_index(VP) * columns
    column_ids = lax.broadcasted_iota(jnp.int32, (total_rows, columns), 1)
    is_target = column_ids == target_col[:, None]

    scores = jnp.dot(rows_all, vocab_matrix, preferred_element_type=f32) + vocab_bias[None, :]
    maxima = jnp.max(scores, axis=1)
    totals = jnp.sum(jnp.exp(scores - maxima[:, None]), axis=1)
    target_score = jnp.sum(jnp.where(is_target, scores, 0.0), axis=1)
    partial_log, target_score = moved(order, [maxima + jnp.log(totals), target_score], (0,))
    count = NZ * NX
    target_score = jnp.pad(target_score.reshape(count, own), ((0, 0), (0, 128 - own)))
    packed = jnp.concatenate(
        [jnp.broadcast_to(partial_log, (count, total_rows)), target_score], axis=1
    )[:, None, :]
    packed = lax.all_to_all(packed, VP, split_axis=0, concat_axis=0, tiled=True)[:, 0]
    each = packed[:, :total_rows]
    maxima = jnp.max(each, axis=0)
    log_total = maxima + jnp.log(jnp.sum(jnp.exp(each - maxima), axis=0))
    own_log = lax.dynamic_slice_in_dim(log_total, lax.axis_index(VP) * own, own)
    own_target = jnp.sum(packed[:, total_rows : total_rows + own], axis=0)
    own_loss = own_log - own_target + penalty * own_log * own_log
    first = lax.axis_index(VP) * columns
    vectors = jnp.concatenate(
        [
            log_total[None],
            loss_weight.T,
            (targets.T - first).astype(f32),
            jnp.zeros((5, total_rows), f32),
        ]
    )
    block = NX * own
    wide = len(FAR) * own
    score_grad, far_own, near, upward, downward, *far_away = pl.pallas_call(
        gradient_kernel,
        out_shape=shaped(
            ((total_rows, columns), bf16),
            ((wide, width), f32),
            ((3 * block, width), f32),
            ((block, width), bf16),
            ((block, width), bf16),
            *[((wide, width), bf16)] * (NX - 1),
        ),
        in_specs=spaces(0, 4),
        out_specs=spaces(0, 5 + NX - 1),
        compiler_params=SMALL,
    )(scores, vocab_matrix, order, vectors)
    from_below = sent_to(upward, "vp_0", 1)
    from_above = sent_to(downward, "vp_0", -1)
    far_x = {kx: sent_to(far_away[kx - 1], "vp_1", kx) for kx in (2, 1, 3)}

    share = width // (NY * NC)
    place = jnp.stack([lax.axis_index("dp_0"), lax.axis_index("dp_1")])
    (other,) = pl.pallas_call(
        other_kernel,
        out_shape=shaped(((NY * share, columns), bf16)),
        in_specs=spaces(1, 2),
        out_specs=spaces(0, 1),
        compiler_params=SMALL,
    )(place, rows_all, score_grad)
    other = taken_from(other, "dp_1", 1)
    vocab_grad, *away = pl.pallas_call(
        chip_kernel,
        out_shape=shaped(
            ((share, columns), f32), *[((share, columns), bf16)] * (NY - 1)
        ),
        in_specs=spaces(1, 3),
        out_specs=spaces(0, NY),
        compiler_params=SMALL,
    )(place, rows_all, score_grad, other)
    chip_y = {k: sent_to(away[k - 1], "dp_0", k) for k in (2, 1, 3)}
    above, below = near[block : 2 * block], near[2 * block :]
    from_below = sent_to((above + from_below.astype(f32)).astype(bf16), "vp_0", 1)
    from_above = sent_to((below + from_above.astype(f32)).astype(bf16), "vp_0", -1)
    far_sum = far_own
    for kx in range(1, NX):
        far_sum = far_sum + far_x[kx].astype(f32)
    far_sum = far_sum.astype(bf16)
    arrived = [sent_to(far_sum[k * own : (k + 1) * own], "vp_0", FAR[k]) for k in (1, 0, 2)]
    close = near[:block] + from_below.astype(f32) + from_above.astype(f32)
    close_half = close.astype(bf16)
    arrived += [sent_to(close_half[kx * own : (kx + 1) * own], "vp_1", kx) for kx in (2, 1, 3)]
    row_grad = close[:own]
    for piece in arrived:
        row_grad = row_grad + piece.astype(f32)

    scaled_grad = norm_gain * row_grad
    norm_grad = inverse_rms * (
        scaled_grad - unit_rows * jnp.mean(scaled_grad * unit_rows, axis=-1, keepdims=True)
    )
    for k in (2, 1, 3):
        vocab_grad = vocab_grad + chip_y[k].astype(f32)
    return (own_loss[:, None], norm_grad[:, None, :], vocab_grad)


def solution(mesh):
    split = Mesh(mesh.devices.reshape(8, 4, 4, 2), ("vp_0", "vp_1", "dp_0", "dp_1"))
    in_specs = (P(VP, DP, None), P(), P(None, VP), P(VP), P(None, DP), P(None, DP))
    out_specs = (P(VP, DP), P(VP, DP, None), P(DP, VP))
    return jax.shard_map(whole, mesh=split, in_specs=in_specs, out_specs=out_specs, check_vma=False)
```

```python
import jax
import jax.numpy as jnp
import numpy as np
from jax import lax
from jax.experimental import pallas as pl
from jax.experimental.pallas import tpu as pltpu
from jax.sharding import Mesh
from jax.sharding import PartitionSpec as P


VP = ("vp_0", "vp_1")
DP = ("dp_0", "dp_1")


epsilon = 1e-06
penalty = 0.005
f32 = jnp.float32
bf16 = jnp.bfloat16

NZ, NX, NY, NC = 8, 4, 4, 2
FAR = (3, 4, 5)


def taken_from(array, axis, step):
    count = lax.axis_size(axis)
    return lax.ppermute(array, axis, [(i, (i - step) % count) for i in range(count)])


def sent_to(array, axis, step):
    return taken_from(array, axis, -step)


def slots(own):
    near = [(kz, kx) for kz in (0, 1, 7) for kx in range(NX)]
    far = [(kz, kx) for kx in range(NX) for kz in FAR]
    ring = [(kz, kx) for kz in (2, 6) for kx in range(NX)]
    return np.array([(kz, kx, r) for kz, kx in near + far + ring for r in range(own)], np.int32)


def three_parts(values):
    high = lax.reduce_precision(values, 8, 7)
    middle = lax.reduce_precision(values - high, 8, 7)
    low = values - high - middle
    return [part.astype(bf16) for part in (high, middle, low)]


def moved(matrix, vectors, dims):
    parts = jnp.stack([part for vector in vectors for part in three_parts(vector)])
    out = lax.dot_general(parts, matrix, (((1,), dims), ((), ())), preferred_element_type=f32)
    return [out[k] + out[k + 1] + out[k + 2] for k in range(0, 3 * len(vectors), 3)]


def column_vectors(order, vectors):
    high = vectors.astype(bf16)
    left = vectors - high.astype(f32)
    middle = left.astype(bf16)
    low = (left - middle.astype(f32)).astype(bf16)
    count = vectors.shape[0]
    parts = jnp.concatenate([high.astype(f32), middle.astype(f32), low.astype(f32)])
    moved_parts = lax.dot_general(
        order, parts.astype(bf16), (((1,), (1,)), ((), ())), preferred_element_type=f32
    )
    return [
        sum(moved_parts[:, k + count * part : k + count * part + 1] for part in range(3))
        for k in range(3)
    ]


def gradient_kernel(
    scores, matrix, order, vectors, grad, far_own, near, upward, downward, *far_away
):
    @pl.when(pl.program_id(0) == 0)
    def first():
        log_total, weights, target = column_vectors(order[...], vectors[...])
        scale = weights * (1.0 + 2.0 * penalty * log_total)
        target = target.astype(jnp.int32)
        rows, width = scores.shape
        step = 128
        for low in range(0, width, step):
            part = slice(low, low + step)
            ids = lax.broadcasted_iota(jnp.int32, (rows, step), 1) + low
            probs = jnp.exp(scores[:, part] - log_total)
            grad[:, part] = (
                scale * probs - jnp.where(ids == target, weights, 0.0)
            ).astype(bf16)

    block, wide = upward.shape[0], far_own.shape[0]
    out = lax.dot_general(
        grad[...], matrix[...], (((1,), (1,)), ((), ())), preferred_element_type=f32
    )
    near[...] = out[: 3 * block]
    at = 3 * block
    far_own[...] = out[at : at + wide]
    for ref in far_away:
        at += wide
        ref[...] = out[at : at + wide].astype(bf16)
    at += wide
    upward[...] = out[at : at + block].astype(bf16)
    downward[...] = out[at + block :].astype(bf16)


def gradients(scores, matrix, order, vectors, block, wide):
    rows, columns = scores.shape
    width = matrix.shape[0]
    step = 512
    kinds = [(wide, f32), (3 * block, f32), (block, bf16), (block, bf16)]
    kinds += [(wide, bf16)] * (NX - 1)
    return pl.pallas_call(
        gradient_kernel,
        grid=(width // step,),
        out_shape=[jax.ShapeDtypeStruct((rows, columns), bf16)]
        + [jax.ShapeDtypeStruct((count, width), kind) for count, kind in kinds],
        in_specs=[
            pl.BlockSpec(scores.shape, lambda i: (0, 0)),
            pl.BlockSpec((step, columns), lambda i: (i, 0)),
            pl.BlockSpec(order.shape, lambda i: (0, 0)),
            pl.BlockSpec(vectors.shape, lambda i: (0, 0)),
        ],
        out_specs=[pl.BlockSpec((rows, columns), lambda i: (0, 0))]
        + [pl.BlockSpec((count, step), lambda i: (0, i)) for count, kind in kinds],
    )(scores, matrix, order, vectors)


def vocab_product(rows, grad, first, share):
    part = pl.ds(pl.multiple_of(first * share, share), share)
    return lax.dot_general(
        rows[:, part], grad[...], (((0,), (0,)), ((), ())), preferred_element_type=f32
    )


def other_kernel(place, rows, grad, out):
    share = rows.shape[1] // (NY * NC)

    def body(y, carry):
        product = vocab_product(rows, grad, y * NC + 1 - place[1], share)
        out[pl.ds(pl.multiple_of(y * share, share), share), :] = product.astype(bf16)
        return carry

    lax.fori_loop(0, NY, body, 0)


def chip_kernel(place, rows, grad, other, own, *away):
    share = rows.shape[1] // (NY * NC)
    for k, ref in enumerate((own, *away)):
        y = lax.rem(place[0] + k, NY)
        product = vocab_product(rows, grad, y * NC + place[1], share)
        product = product + other[pl.ds(pl.multiple_of(y * share, share), share), :].astype(f32)
        ref[...] = product.astype(ref.dtype)


def shaped(*shapes):
    return tuple(jax.ShapeDtypeStruct(dims, kind) for dims, kind in shapes)


def spaces(scalars, arrays):
    return [pl.BlockSpec(memory_space=pltpu.SMEM)] * scalars + [
        pl.BlockSpec(memory_space=pltpu.VMEM)
    ] * arrays


def whole(hidden_rows, norm_gain, vocab_matrix, vocab_bias, targets, loss_weight):
    inputs = hidden_rows[:, 0, :].astype(f32)
    inverse_rms = lax.rsqrt(jnp.mean(inputs * inputs, axis=-1, keepdims=True) + epsilon)
    unit_rows = inputs * inverse_rms
    normed = (unit_rows * norm_gain).astype(bf16)
    own, width = normed.shape
    total_rows = own * NZ * NX
    columns = vocab_matrix.shape[1]

    along_x = {kx: taken_from(normed, "vp_1", kx) for kx in (1, 3, 2)}
    straight = {kz: taken_from(normed, "vp_0", kz) for kz in (4, 3, 5)}
    line = jnp.concatenate([normed] + [along_x[kx] for kx in range(1, NX)])
    up1 = taken_from(line, "vp_0", 1)
    down1 = taken_from(line, "vp_0", -1)
    three = lax.optimization_barrier(jnp.concatenate([straight[kz] for kz in FAR]))
    threes = {kx: taken_from(three, "vp_1", kx) for kx in (2, 1, 3)}
    up2 = taken_from(up1, "vp_0", 1)
    down2 = taken_from(down1, "vp_0", -1)
    place_z, place_x = lax.axis_index("vp_0"), lax.axis_index("vp_1")
    place = slots(own)
    owner = (place_z + place[:, 0]) % NZ * NX + (place_x + place[:, 1]) % NX
    index = owner * own + place[:, 2]
    ids = lax.broadcasted_iota(jnp.int32, (total_rows, total_rows), 1)
    order = (index[:, None] == ids).astype(bf16)

    target_col, _ = moved(
        order, [targets[:, 0].astype(f32), loss_weight[:, 0]], (1,)
    )
    target_col = target_col.astype(jnp.int32) - lax.axis_index(VP) * columns
    *early, target_col = lax.optimization_barrier((line, up1, down1, three, target_col))
    late = [threes[kx] for kx in range(1, NX)] + [up2, down2]
    rows_all = jnp.concatenate(early + late)
    column_ids = lax.broadcasted_iota(jnp.int32, (total_rows, columns), 1)
    is_target = column_ids == target_col[:, None]

    scores = jnp.dot(rows_all, vocab_matrix, preferred_element_type=f32) + vocab_bias[None, :]
    maxima = jnp.max(scores, axis=1)
    totals = jnp.sum(jnp.exp(scores - maxima[:, None]), axis=1)
    target_score = jnp.sum(jnp.where(is_target, scores, 0.0), axis=1)
    partial_log, target_score = moved(order, [maxima + jnp.log(totals), target_score], (0,))
    count = NZ * NX
    target_score = jnp.pad(target_score.reshape(count, own), ((0, 0), (0, 128 - own)))
    packed = jnp.concatenate(
        [jnp.broadcast_to(partial_log, (count, total_rows)), target_score], axis=1
    )[:, None, :]
    packed = lax.all_to_all(packed, VP, split_axis=0, concat_axis=0, tiled=True)[:, 0]
    each = packed[:, :total_rows]
    maxima = jnp.max(each, axis=0)
    log_total = maxima + jnp.log(jnp.sum(jnp.exp(each - maxima), axis=0))
    own_log = lax.dynamic_slice_in_dim(log_total, lax.axis_index(VP) * own, own)
    own_target = jnp.sum(packed[:, total_rows : total_rows + own], axis=0)
    own_loss = own_log - own_target + penalty * own_log * own_log
    first = lax.axis_index(VP) * columns
    vectors = jnp.concatenate(
        [
            log_total[None],
            loss_weight.T,
            (targets.T - first).astype(f32),
            jnp.zeros((5, total_rows), f32),
        ]
    )
    block = NX * own
    wide = len(FAR) * own
    score_grad, far_own, near, upward, downward, *far_away = gradients(
        scores, vocab_matrix, order, vectors, block, wide
    )
    from_below = sent_to(upward, "vp_0", 1)
    from_above = sent_to(downward, "vp_0", -1)
    far_x = {kx: sent_to(far_away[kx - 1], "vp_1", kx) for kx in (2, 1, 3)}

    share = width // (NY * NC)
    place = jnp.stack([lax.axis_index("dp_0"), lax.axis_index("dp_1")])
    (other,) = pl.pallas_call(
    other_kernel,
    out_shape=shaped(((NY * share, columns), bf16)),
    in_specs=spaces(1, 2),
    out_specs=spaces(0, 1),
    )(place, rows_all, score_grad)
    other = taken_from(other, "dp_1", 1)
    vocab_grad, *away = pl.pallas_call(
    chip_kernel,
    out_shape=shaped(
        ((share, columns), f32), *[((share, columns), bf16)] * (NY - 1)
    ),
    in_specs=spaces(1, 3),
    out_specs=spaces(0, NY),
    )(place, rows_all, score_grad, other)
    chip_y = {k: sent_to(away[k - 1], "dp_0", k) for k in (2, 1, 3)}
    above, below = near[block : 2 * block], near[2 * block :]
    from_below = sent_to((above + from_below.astype(f32)).astype(bf16), "vp_0", 1)
    from_above = sent_to((below + from_above.astype(f32)).astype(bf16), "vp_0", -1)
    far_sum = far_own
    for kx in range(1, NX):
        far_sum = far_sum + far_x[kx].astype(f32)
    far_sum = far_sum.astype(bf16)
    arrived = [sent_to(far_sum[k * own : (k + 1) * own], "vp_0", FAR[k]) for k in (1, 0, 2)]
    close = near[:block] + from_below.astype(f32) + from_above.astype(f32)
    close_half = close.astype(bf16)
    arrived += [sent_to(close_half[kx * own : (kx + 1) * own], "vp_1", kx) for kx in (2, 1, 3)]
    row_grad = close[:own]
    for piece in arrived:
        row_grad = row_grad + piece.astype(f32)

    scaled_grad = norm_gain * row_grad
    norm_grad = inverse_rms * (
        scaled_grad - unit_rows * jnp.mean(scaled_grad * unit_rows, axis=-1, keepdims=True)
    )
    for k in (2, 1, 3):
        vocab_grad = vocab_grad + chip_y[k].astype(f32)
    return (own_loss[:, None], norm_grad[:, None, :], vocab_grad)


def solution(mesh):
    split = Mesh(mesh.devices.reshape(8, 4, 4, 2), ("vp_0", "vp_1", "dp_0", "dp_1"))
    in_specs = (P(VP, DP, None), P(), P(None, VP), P(VP), P(None, DP), P(None, DP))
    out_specs = (P(VP, DP), P(VP, DP, None), P(DP, VP))
    return jax.shard_map(whole, mesh=split, in_specs=in_specs, out_specs=out_specs, check_vma=False)
```
